32 devices in a mesh: grp: 2 (over x), fs: 4 (over y, core), tp: 4 (over z).
Axes of the slice: x: 2, y: 2, z: 4, core: 2. Of those that a mesh axis runs over, the one named last changes fastest.
Arguments:
- stream: bfloat16 [4096, 2048], P(('grp', 'fs', 'tp')), parts along dimension 0, may hold values from -4 to 4
- gain_first: bfloat16 [2048], replicated, may hold values from 0.099609375 to 1.8984375
- gate_first: bfloat16 [2048, 4096], P('fs', 'tp'), may hold values from -0.125 to 0.125
- up_first: bfloat16 [2048, 4096], P('fs', 'tp'), may hold values from -0.125 to 0.125
- down_first: bfloat16 [4096, 2048], P('tp', 'fs'), may hold values from -0.09375 to 0.09375
- gain_second: bfloat16 [2048], replicated, may hold values from 0.099609375 to 1.8984375
- gate_second: bfloat16 [2048, 4096], P('fs', 'tp'), may hold values from -0.125 to 0.125
- up_second: bfloat16 [2048, 4096], P('fs', 'tp'), may hold values from -0.125 to 0.125
- down_second: bfloat16 [4096, 2048], P('tp', 'fs'), may hold values from -0.09375 to 0.09375
Outputs:
- result: bfloat16 [4096, 2048], P(('grp', 'fs', 'tp')), parts along dimension 0
The draws below stay inside these ranges and needn't reach their ends.
There are 2 independent parts, one for each index of `grp`. The reference program is written for one: setup_inputs(seed, part) draws one part's arguments, and reference() takes and returns one part's arrays. A program takes and returns all parts, laid end to end along the dimension named above; an argument that names none is the same for every part. Nothing has to cross between parts.
All inputs are finite; a program needn't handle non-finite values.
Results may differ from the reference program's by a relative error of at most 0.018.
Values may be sent and summed in bfloat16 or wider, within the bound.
No kernel may reach another device: no remote copies, remote signals or barrier semaphores. Data moves between devices by JAX's collectives and lax.ppermute only.
A program may use at most 64 MiB of HBM per device.

```python
import jax
import jax.numpy as jnp
from jax import lax

D = 2048
FF = 4096
TOKENS = 2048
N_TP = 4


def block_scale(rng, extent, shards, smallest, largest):
    level = 1.0
    for position, blocks in shards:
        steps = jax.random.uniform(jax.random.fold_in(jax.random.fold_in(rng, 6), position), (blocks,), jnp.float32, smallest / len(shards), largest / len(shards))
        level = level * jnp.repeat(jnp.exp(steps), extent[position] // blocks).reshape((-1,) + (1,) * (len(extent) - 1 - position))
    return level


def scatter_about(stream_key, dims, deviation, bound, cuts=(), kind=jnp.bfloat16):
    drawn = deviation * jax.random.normal(stream_key, dims, jnp.float32)
    if cuts:
        drawn = drawn * block_scale(stream_key, dims, cuts, -0.22, 0.18)
    return jnp.clip(drawn, -bound, bound).astype(kind)


def setup_inputs(seed: int = 0, part: int = 0) -> dict:
    streams_of = jax.random.split(jax.random.key(seed), 10)
    part_keys = jax.random.split(jax.random.fold_in(streams_of[9], part), 10)
    return {
        "stream": scatter_about(part_keys[0], (TOKENS, D), 0.5, 4.0, ((0, 16),)),
        "gain_first": jnp.clip(1.0 + 0.18 * jax.random.normal(streams_of[1], (D,), jnp.float32), 0.099609375, 1.8984375).astype(jnp.bfloat16),
        "gate_first": scatter_about(streams_of[2], (D, FF), D ** -0.5, 0.125, ((0, 4), (1, 4))),
        "up_first": scatter_about(streams_of[3], (D, FF), D ** -0.5, 0.125, ((0, 4), (1, 4))),
        "down_first": scatter_about(streams_of[4], (FF, D), FF ** -0.5, 0.09375, ((0, 4), (1, 4))),
        "gain_second": jnp.clip(1.0 + 0.18 * jax.random.normal(streams_of[5], (D,), jnp.float32), 0.099609375, 1.8984375).astype(jnp.bfloat16),
        "gate_second": scatter_about(streams_of[6], (D, FF), D ** -0.5, 0.125, ((0, 4), (1, 4))),
        "up_second": scatter_about(streams_of[7], (D, FF), D ** -0.5, 0.125, ((0, 4), (1, 4))),
        "down_second": scatter_about(streams_of[8], (FF, D), FF ** -0.5, 0.09375, ((0, 4), (1, 4))),
    }


def half_branch(stream, gain, w_gate, w_up, w_down):
    stream_f = stream.astype(jnp.float32)
    normed = (stream_f * lax.rsqrt(lax.optimization_barrier(jnp.mean(stream_f * stream_f, axis=-1, keepdims=True)) + 1e-06) * gain.astype(jnp.float32)).astype(jnp.bfloat16)
    gate_act = jnp.dot(normed, w_gate, preferred_element_type=jnp.float32)
    up_act = jnp.dot(normed, w_up, preferred_element_type=jnp.float32)
    hidden = (jax.nn.silu(gate_act) * up_act).astype(jnp.bfloat16)
    span_width = FF // N_TP
    summed = jnp.zeros(stream.shape, jnp.float32)
    for shard in range(N_TP):
        partial_sum = jnp.dot(hidden[:, shard * span_width:(shard + 1) * span_width], w_down[shard * span_width:(shard + 1) * span_width], preferred_element_type=jnp.float32).astype(jnp.bfloat16)
        partial_sum = lax.optimization_barrier(partial_sum)
        summed = summed + partial_sum.astype(jnp.float32)
    return (stream_f + 0.5 * summed).astype(jnp.bfloat16)

def reference(stream, gain_first, gate_first, up_first, down_first, gain_second, gate_second, up_second, down_second):
    middle = half_branch(stream, gain_first, gate_first, up_first, down_first)
    return half_branch(middle, gain_second, gate_second, up_second, down_second)
```

```python
import jax
import jax.numpy as jnp
from jax import lax
from jax.sharding import PartitionSpec as P


CORES = 2


def line_gather(v, axis, n, pos, stride=1):
    def pairs(srcs, step):
        return [(j * stride + c, (j + step) * stride + c) for j in srcs for c in range(stride)]

    if n == 1:
        return [v]
    if n == 2:
        return [v, lax.ppermute(v, axis, pairs([0], 1) + pairs([1], -1))]
    right, left = [v], [v]
    for k in range(1, n):
        right.append(lax.ppermute(right[-1], axis, pairs(range(k - 1, n - 1), 1)))
        left.append(lax.ppermute(left[-1], axis, pairs(range(1, n - k + 1), -1)))
    return [v] + [jnp.where(pos >= k, right[k], left[n - k]) for k in range(1, n)]


def line_scatter(parts, axis, n):
    acc_r = acc_l = None

    def join(part, acc):
        if acc is None:
            return part
        return (part.astype(jnp.float32) + acc.astype(jnp.float32)).astype(part.dtype)

    for d in range(n - 1, 0, -1):
        acc_r = lax.ppermute(join(parts[n - d], acc_r), axis, [(j, j + 1) for j in range(n - d)])
        acc_l = lax.ppermute(join(parts[d], acc_l), axis, [(j, j - 1) for j in range(d, n)])
    total = parts[0].astype(jnp.float32)
    for acc in (acc_r, acc_l):
        if acc is not None:
            total = total + acc.astype(jnp.float32)
    return total


def gather_weight(w, dim, n_grp, n_fs, g, y):
    ny = n_fs // CORES
    other_core = [(j, j ^ 1) for j in range(n_fs)]
    width = w.shape[dim] // n_grp
    half = lax.dynamic_slice_in_dim(w, g * width, width, dim)
    slots = line_gather(half, "fs", ny, y, CORES)
    pieces = [w, lax.ppermute(w, "fs", other_core)]
    for k in range(1, ny):
        mine = [slots[k]] + [
            lax.ppermute(slots[k], "grp", [(j, (j + b) % n_grp) for j in range(n_grp)])
            for b in range(1, n_grp)
        ]
        pieces += mine + [lax.ppermute(m, "fs", other_core) for m in mine]
    return jnp.concatenate(pieces, axis=dim)


def block_order(n_grp, n_fs, g, f):
    ny = n_fs // CORES
    y, c = f // CORES, f % CORES

    def own(k, cc, b):
        part = b if k == 0 else (g - b) % n_grp
        return (((y - k) % ny) * CORES + (c ^ cc)) * n_grp + part

    def back(yy, cc, h):
        k = (y - yy) % ny
        b = jnp.where(k == 0, h, (g - h) % n_grp)
        return (k * CORES + (c ^ cc)) * n_grp + b

    index = [(a, cc, b) for a in range(ny) for cc in range(CORES) for b in range(n_grp)]
    return [own(*i) for i in index], [back(*i) for i in index]


def reorder(v, order):
    width = v.shape[-1] // len(order)
    return jnp.concatenate(
        [lax.dynamic_slice_in_dim(v, o * width, width, v.ndim - 1) for o in order], axis=-1
    )


def half_branch(stream, gain, w_gate, w_up, w_down, n_tp, t):
    stream_f = stream.astype(jnp.float32)
    normed = (
        stream_f
        * lax.rsqrt(jnp.mean(stream_f * stream_f, axis=-1, keepdims=True) + 1e-06)
        * gain.astype(jnp.float32)
    ).astype(jnp.bfloat16)
    rows = stream.shape[0]
    tokens = jnp.concatenate(line_gather(normed, "tp", n_tp, t), axis=0)
    gate_act = jnp.dot(tokens, w_gate, preferred_element_type=jnp.float32)
    up_act = jnp.dot(tokens, w_up, preferred_element_type=jnp.float32)
    hidden = (jax.nn.silu(gate_act) * up_act).astype(jnp.bfloat16)
    partial = jnp.dot(hidden, w_down, preferred_element_type=jnp.float32).astype(jnp.bfloat16)
    parts = [partial[k * rows:(k + 1) * rows] for k in range(n_tp)]
    summed = line_scatter(parts, "tp", n_tp)
    return (stream_f + 0.5 * summed).astype(jnp.bfloat16)


def solution(mesh):
    n_grp, n_fs, n_tp = (mesh.shape[a] for a in ("grp", "fs", "tp"))

    def local(stream, gain_first, gate_first, up_first, down_first,
              gain_second, gate_second, up_second, down_second):
        g, f, t = (lax.axis_index(a) for a in ("grp", "fs", "tp"))
        y = f // CORES
        to_own, to_natural = block_order(n_grp, n_fs, g, f)
        stream = reorder(stream, to_own)
        gain_first, gain_second = reorder(gain_first, to_own), reorder(gain_second, to_own)

        def full(w, dim):
            return gather_weight(w, dim, n_grp, n_fs, g, y)

        first = full(gate_first, 0), full(up_first, 0), full(down_first, 1)
        second = full(gate_second, 0), full(up_second, 0), full(down_second, 1)
        middle = half_branch(stream, gain_first, *first, n_tp, t)
        result = half_branch(middle, gain_second, *second, n_tp, t)
        return reorder(result, to_natural)

    in_specs = (
        P(("grp", "fs", "tp"), None),
        P(),
        P("fs", "tp"),
        P("fs", "tp"),
        P("tp", "fs"),
        P(),
        P("fs", "tp"),
        P("fs", "tp"),
        P("tp", "fs"),
    )
    out_specs = P(("grp", "fs", "tp"), None)
    return jax.shard_map(local, mesh=mesh, in_specs=in_specs, out_specs=out_specs, check_vma=False)
```

```python
import functools

import jax
import jax.numpy as jnp
import numpy as np
from jax import lax
from jax.experimental import pallas as pl
from jax.experimental.pallas import tpu as pltpu
from jax.sharding import PartitionSpec as P


CORES = 2
LANES = 128
CHUNKS = 1
F32, BF16 = jnp.float32, jnp.bfloat16
VMEM = pl.BlockSpec(memory_space=pltpu.VMEM)
SMEM = pl.BlockSpec(memory_space=pltpu.SMEM)


def line_gather(v, axis, n, stride=1):
    def pairs(srcs, step):
        return [(j * stride + c, (j + step) * stride + c) for j in srcs for c in range(stride)]

    if n == 2:
        return [v, lax.ppermute(v, axis, pairs([0], 1) + pairs([1], -1))], None
    right, left = [v], [v]
    for k in range(1, n):
        right.append(lax.ppermute(right[-1], axis, pairs(range(k - 1, n - 1), 1)))
        left.append(lax.ppermute(left[-1], axis, pairs(range(1, n - k + 1), -1)))
    return right, left


def line_slots(right, left, n, pos):
    if left is None:
        return right
    return right[:1] + [jnp.where(pos >= k, right[k], left[n - k]) for k in range(1, n)]


def line_scatter(parts, axis, n):
    acc_r = acc_l = None

    def join(part, acc):
        if acc is None:
            return part
        return (part.astype(F32) + acc.astype(F32)).astype(part.dtype)

    for d in range(n - 1, 0, -1):
        acc_r = lax.ppermute(join(parts[n - d], acc_r), axis, [(j, j + 1) for j in range(n - d)])
        acc_l = lax.ppermute(join(parts[d], acc_l), axis, [(j, j - 1) for j in range(d, n)])
    return [parts[0]] + [acc for acc in (acc_r, acc_l) if acc is not None]


def gather_weight(w, dim, n_grp, n_fs, g, y):
    ny = n_fs // CORES
    other_core = [(j, j ^ 1) for j in range(n_fs)]
    width = w.shape[dim] // n_grp
    half = lax.dynamic_slice_in_dim(w, g * width, width, dim)
    slots = line_slots(*line_gather(half, "fs", ny, CORES), ny, y)
    pieces = [w, lax.ppermute(w, "fs", other_core)]
    for k in range(1, ny):
        mine = [slots[k]] + [
            lax.ppermute(slots[k], "grp", [(j, (j + b) % n_grp) for j in range(n_grp)])
            for b in range(1, n_grp)
        ]
        pieces += mine + [lax.ppermute(m, "fs", other_core) for m in mine]
    return pieces


def block_order(n_grp, n_fs, g, f):
    ny = n_fs // CORES
    y, c = f // CORES, f % CORES
    a, cc, b = (jnp.asarray(i.reshape(-1), jnp.int32) for i in np.indices((ny, CORES, n_grp)))
    own = (((y - a) % ny) * CORES + (c ^ cc)) * n_grp + jnp.where(a == 0, b, (g - b) % n_grp)
    k = (y - a) % ny
    back = (k * CORES + (c ^ cc)) * n_grp + jnp.where(k == 0, b, (g - b) % n_grp)
    return own.astype(jnp.int32), back.astype(jnp.int32)


def reorder(v, order):
    width = v.shape[-1] // order.shape[0]
    return jnp.concatenate(
        [lax.dynamic_slice_in_dim(v, order[s] * width, width, v.ndim - 1) for s in range(order.shape[0])],
        axis=-1,
    )


def at(order_ref, s, width):
    return pl.ds(pl.multiple_of(order_ref[s] * width, width), width)


def enter_body(order_ref, x_ref, gain_ref, *outs):
    half = len(outs) // 2
    n = order_ref.shape[0]
    width = x_ref.shape[1] // n
    x = x_ref[...].astype(F32)
    scale = lax.rsqrt(jnp.mean(x * x, axis=-1, keepdims=True) + 1e-06)
    rows = x_ref.shape[0] // half
    for s in range(n):
        src, dst = at(order_ref, s, width), slice(s * width, (s + 1) * width)
        piece = x_ref[:, src]
        normed = (piece.astype(F32) * scale * gain_ref[:, src]).astype(BF16)
        for q in range(half):
            outs[q][:, dst] = normed[q * rows:(q + 1) * rows]
            outs[half + q][:, dst] = piece[q * rows:(q + 1) * rows]


def middle_body(order_ref, gain_ref, x_ref, *refs):
    terms, (normed_ref, mid_ref) = refs[:-2], refs[-2:]
    n = order_ref.shape[0]
    width = x_ref.shape[1] // n
    total = terms[0][...].astype(F32)
    for t in terms[1:]:
        total = total + t[...].astype(F32)
    mid = (x_ref[...].astype(F32) + 0.5 * total).astype(BF16)
    mid_ref[...] = mid
    m = mid.astype(F32)
    m = m * lax.rsqrt(jnp.mean(m * m, axis=-1, keepdims=True) + 1e-06)
    for s in range(n):
        dst = slice(s * width, (s + 1) * width)
        normed_ref[:, dst] = (m[:, dst] * gain_ref[:, at(order_ref, s, width)]).astype(BF16)


def leave_body(order_ref, x_ref, *refs):
    terms, out_ref = refs[:-1], refs[-1]
    n = order_ref.shape[0]
    width = x_ref.shape[1] // n
    for s in range(n):
        src = slice(s * width, (s + 1) * width)
        total = terms[0][:, src].astype(F32)
        for t in terms[1:]:
            total = total + t[:, src].astype(F32)
        out_ref[:, at(order_ref, s, width)] = (x_ref[:, src].astype(F32) + 0.5 * total).astype(BF16)


def small_call(body, order, args, outs):
    return pl.pallas_call(
        body,
        in_specs=[SMEM] + [VMEM] * len(args),
        out_specs=[VMEM] * len(outs),
        out_shape=[jax.ShapeDtypeStruct(s, BF16) for s in outs],
    )(order, *args)


def up_body(pos_ref, *refs, n, n_pieces):
    n_tok = 2 * n - 1 if n > 2 else n
    toks = refs[:n_tok]
    gates = refs[n_tok:n_tok + n_pieces]
    ups = refs[n_tok + n_pieces:n_tok + 2 * n_pieces]
    out_ref, all_ref = refs[-2:]
    rows = toks[0].shape[0]

    @pl.when(pl.program_id(0) == 0)
    def _():
        all_ref[0:rows] = toks[0][...]
        for k in range(1, n):
            dst = slice(k * rows, (k + 1) * rows)
            if n == 2:
                all_ref[dst] = toks[1][...]
                continue

            @pl.when(pos_ref[0] >= k)
            def _():
                all_ref[dst] = toks[k][...]

            @pl.when(pos_ref[0] < k)
            def _():
                all_ref[dst] = toks[n - 1 + n - k][...]

    def product(pieces):
        acc, base = None, 0
        for p in pieces:
            part = jnp.dot(all_ref[:, base:base + p.shape[0]], p[...], preferred_element_type=F32)
            acc = part if acc is None else acc + part
            base += p.shape[0]
        return acc

    gate, up = product(gates), product(ups)
    out_ref[...] = (gate / (1.0 + jnp.exp(-gate)) * up).astype(BF16)


def up_call(pos, toks, gates, ups, n):
    rows, d = toks[0].shape
    ff = gates[0].shape[1]
    tile = 256
    whole = lambda a: pl.BlockSpec(a.shape, lambda i: (0, 0))
    cols = lambda a: pl.BlockSpec((a.shape[0], tile), lambda i: (0, i))
    return pl.pallas_call(
        functools.partial(up_body, n=n, n_pieces=len(gates)),
        grid=(ff // tile,),
        in_specs=[SMEM] + [whole(a) for a in toks] + [cols(a) for a in gates + ups],
        out_specs=pl.BlockSpec((n * rows, tile), lambda i: (0, i)),
        out_shape=jax.ShapeDtypeStruct((n * rows, ff), BF16),
        scratch_shapes=[pltpu.VMEM((n * rows, d), BF16)],
        cost_estimate=pl.CostEstimate(
            flops=4 * n * rows * d * ff, transcendentals=n * rows * ff,
            bytes_accessed=4 * d * ff + 4 * n * rows * d),
        name="gate_up",
    )(pos, *toks, *gates, *ups)


def down_body(hidden_ref, *refs, n):
    pieces, outs = refs[:-n], refs[-n:]
    rows = outs[0].shape[0]
    base = 0
    for p in pieces:
        width = p.shape[1]
        part = jnp.dot(hidden_ref[...], p[...], preferred_element_type=F32).astype(BF16)
        dst = pl.ds(pl.multiple_of(base + pl.program_id(0) * width, LANES), width)
        for k in range(n):
            outs[k][:, dst] = part[k * rows:(k + 1) * rows]
        base += width * STEPS


STEPS = 2


def down_call(hidden, pieces, n):
    total, ff = hidden.shape
    rows = total // n
    d = sum(p.shape[1] for p in pieces)
    return pl.pallas_call(
        functools.partial(down_body, n=n),
        grid=(STEPS,),
        in_specs=[pl.BlockSpec(hidden.shape, lambda i: (0, 0))]
        + [pl.BlockSpec((ff, p.shape[1] // STEPS), lambda i: (0, i)) for p in pieces],
        out_specs=[pl.BlockSpec((rows, d), lambda i: (0, 0))] * n,
        out_shape=[jax.ShapeDtypeStruct((rows, d), BF16)] * n,
        cost_estimate=pl.CostEstimate(
            flops=2 * total * d * ff, transcendentals=0,
            bytes_accessed=2 * d * ff + 2 * total * (d + ff)),
        name="down",
    )(hidden, *pieces)


def solution(mesh):
    n_grp, n_fs, n_tp = (mesh.shape[a] for a in ("grp", "fs", "tp"))

    def local(stream, gain_first, gate_first, up_first, down_first,
              gain_second, gate_second, up_second, down_second):
        g, f, t = (lax.axis_index(a) for a in ("grp", "fs", "tp"))
        y = f // CORES
        pos = t.astype(jnp.int32).reshape(1)
        rows, d = stream.shape
        to_own, to_natural = block_order(n_grp, n_fs, g, f)
        blocked = (d // to_own.shape[0]) % (STEPS * LANES) == 0
        gains = gain_first, gain_second
        if not blocked:
            stream = reorder(stream, to_own)
            gains = tuple(reorder(gain, to_own) for gain in gains)
            order = jnp.zeros((1,), jnp.int32)
        else:
            order = to_own
        gains = tuple(gain.astype(F32).reshape(1, d) for gain in gains)

        def full(w, dim):
            pieces = gather_weight(w, dim, n_grp, n_fs, g, y)
            return pieces if blocked else [jnp.concatenate(pieces, axis=dim)]

        first = full(gate_first, 0), full(up_first, 0), full(down_first, 1)
        second = full(gate_second, 0), full(up_second, 0), full(down_second, 1)
        part = (rows // CHUNKS, d)

        def branch(normed, weights):
            right, left = line_gather(normed, "tp", n_tp)
            toks = right + (left[1:] if left is not None else [])
            hidden = up_call(pos, toks, weights[0], weights[1], n_tp)
            parts = down_call(hidden, weights[2], n_tp)
            return line_scatter(parts, "tp", n_tp)

        entered = small_call(enter_body, order, (stream, gains[0]), [part] * (2 * CHUNKS))
        results = []
        for q in range(CHUNKS):
            normed, own = entered[q], entered[CHUNKS + q]
            terms = branch(normed, first)
            normed, own = small_call(middle_body, order, (gains[1], own, *terms), [part] * 2)
            terms = branch(normed, second)
            results += small_call(leave_body, order, (own, *terms), [part])
        result = jnp.concatenate(results, axis=0) if CHUNKS > 1 else results[0]
        return result if blocked else reorder(result, to_natural)

    in_specs = (
        P(("grp", "fs", "tp"), None),
        P(),
        P("fs", "tp"),
        P("fs", "tp"),
        P("tp", "fs"),
        P(),
        P("fs", "tp"),
        P("fs", "tp"),
        P("tp", "fs"),
    )
    out_specs = P(("grp", "fs", "tp"), None)
    return jax.shard_map(local, mesh=mesh, in_specs=in_specs, out_specs=out_specs, check_vma=False)
```
